512 devices in a mesh: tp: 32 (over z, x), dp: 16 (over y, core).
Axes of the slice: x: 4, y: 8, z: 8, core: 2. Of those that a mesh axis runs over, the one named last changes fastest.
Arguments:
- tokens: bfloat16 [256, 4096], P('dp', 'tp'), may hold values from -6 to 6
- norm_gain: float32 [2, 4096], replicated, may hold values from 0.1 to 1.9
- w_in: bfloat16 [2, 4096, 2048], P(None, 'dp', 'tp'), may hold values from -0.09375 to 0.09375
- w_gate: bfloat16 [2, 4096, 2048], P(None, 'dp', 'tp'), may hold values from -0.1875 to 0.1875
- decay_rate: float32 [2, 128, 64], P(None, 'tp'), may hold values from 0.05 to 2
- frequency: float32 [2, 128, 64], P(None, 'tp'), may hold values from -3 to 3
- log_step: float32 [2, 128], P(None, 'tp'), may hold values from -3 to 0
- map_re: float32 [2, 128, 16, 64], P(None, 'tp'), may hold values from -1.5 to 1.5
- map_im: float32 [2, 128, 16, 64], P(None, 'tp'), may hold values from -1.5 to 1.5
- read_re: float32 [2, 128, 16, 64], P(None, 'tp'), may hold values from -0.5 to 0.5
- read_im: float32 [2, 128, 16, 64], P(None, 'tp'), may hold values from -0.5 to 0.5
- skip_weight: float32 [2, 128, 16], P(None, 'tp'), may hold values from -4 to 4
- w_out: bfloat16 [2, 2048, 4096], P(None, 'dp', 'tp'), may hold values from -0.25 to 0.25
- state_re: float32 [2, 256, 128, 64], P(None, 'dp', 'tp'), may hold values from -6 to 6
- state_im: float32 [2, 256, 128, 64], P(None, 'dp', 'tp'), may hold values from -6 to 6
Outputs:
- hidden: bfloat16 [256, 4096], P('dp', 'tp')
- new_re: float32 [2, 256, 128, 64], P(None, 'dp', 'tp')
- new_im: float32 [2, 256, 128, 64], P(None, 'dp', 'tp')
The draws below stay inside these ranges and needn't reach their ends.
All inputs are finite; a program needn't handle non-finite values.
Results may differ from the reference program's by a relative error of at most 0.01.
Values may be sent and summed in bfloat16 or wider, within the bound.
No kernel may reach another device: no remote copies, remote signals or barrier semaphores. Data moves between devices by JAX's collectives and lax.ppermute only.
A program may use at most 64 MiB of HBM per device.

```python
import math
import jax
import jax.numpy as jnp
from jax import lax

D = 4096
GROUPS = 128
GROUP_CH = 16
STATE_N = 64
LAYERS = 2
WIDTH = 2048
SEQS = 256


def block_scale(rng, extent, cuts, smallest, high):
    def one(position, blocks):
        heights = jax.random.uniform(jax.random.fold_in(jax.random.fold_in(rng, 6), position), (blocks,), jnp.float32, smallest / len(cuts), high / len(cuts))
        return jnp.repeat(jnp.exp(heights), extent[position] // blocks).reshape((-1,) + (1,) * (len(extent) - position - 1))

    loudness = one(*cuts[0])
    for cut in cuts[1:]:
        loudness = loudness * one(*cut)
    return loudness


def normal_values(own_key, extent, deviation, reach, shards=(), dtype=jnp.bfloat16):
    result = deviation * jax.random.normal(own_key, extent, jnp.float32)
    if shards:
        result = result * block_scale(own_key, extent, shards, -0.22, 0.18)
    return jnp.clip(result, -reach, reach).astype(dtype)


def setup_inputs(seed: int = 0) -> dict:
    streams_of = jax.random.split(jax.random.key(seed), 16)
    return {
        "tokens": normal_values(streams_of[0], (SEQS, D), 1.0, 6.0, ((0, 16), (1, 32))),
        "norm_gain": jnp.clip(1.0 + 0.18 * jax.random.normal(streams_of[1], (LAYERS, D), jnp.float32), 0.1, 1.9),
        "w_in": normal_values(streams_of[2], (LAYERS, D, WIDTH), D ** -0.5, 0.09375, ((1, 16), (2, 32))),
        "w_gate": normal_values(streams_of[3], (LAYERS, D, WIDTH), (D // 4) ** -0.5, 0.1875, ((1, 16), (2, 32))),
        "decay_rate": jnp.clip(jnp.exp(math.log(2.0) - 3.6888794 * jax.random.uniform(streams_of[4], (LAYERS, GROUPS, STATE_N), jnp.float32) ** block_scale(streams_of[4], (LAYERS, GROUPS, STATE_N), ((1, 32),), -0.2, 0.2)), 0.05, 2.0),
        "frequency": jnp.clip(jax.random.uniform(streams_of[5], (LAYERS, GROUPS, STATE_N), jnp.float32, -3.0, 3.0) * block_scale(streams_of[5], (LAYERS, GROUPS, STATE_N), ((1, 32),), -0.4, 0.0), -3.0, 3.0),
        "log_step": jnp.clip(-3.0 + 3.0 * jax.random.uniform(streams_of[6], (LAYERS, GROUPS), jnp.float32) ** block_scale(streams_of[6], (LAYERS, GROUPS), ((1, 32),), -0.2, 0.2), -3.0, 0.0),
        "map_re": normal_values(streams_of[7], (LAYERS, GROUPS, GROUP_CH, STATE_N), GROUP_CH ** -0.5, 1.5, ((1, 32),), jnp.float32),
        "map_im": normal_values(streams_of[8], (LAYERS, GROUPS, GROUP_CH, STATE_N), GROUP_CH ** -0.5, 1.5, ((1, 32),), jnp.float32),
        "read_re": normal_values(streams_of[9], (LAYERS, GROUPS, GROUP_CH, STATE_N), (2 * STATE_N) ** -0.5, 0.5, ((1, 32),), jnp.float32),
        "read_im": normal_values(streams_of[10], (LAYERS, GROUPS, GROUP_CH, STATE_N), (2 * STATE_N) ** -0.5, 0.5, ((1, 32),), jnp.float32),
        "skip_weight": normal_values(streams_of[11], (LAYERS, GROUPS, GROUP_CH), 1.0, 4.0, ((1, 32),), jnp.float32),
        "w_out": normal_values(streams_of[12], (LAYERS, WIDTH, D), (WIDTH // 4) ** -0.5, 0.25, ((1, 16), (2, 32))),
        "state_re": normal_values(streams_of[13], (LAYERS, SEQS, GROUPS, STATE_N), 1.0, 6.0, ((1, 16), (2, 32)), jnp.float32),
        "state_im": normal_values(streams_of[14], (LAYERS, SEQS, GROUPS, STATE_N), 1.0, 6.0, ((1, 16), (2, 32)), jnp.float32),
    }


EPSILON = 1e-06
HIGH = lax.Precision.HIGHEST

def state_update(inputs, old_re, old_im, decay_rate, frequency, log_step, map_re, map_im, read_re, read_im, skip_weight):
    lam_re = -decay_rate
    lam_im = frequency
    step_size = jnp.exp(log_step)[:, None]
    magnitude = jnp.exp(lam_re * step_size)
    decay_re = magnitude * jnp.cos(lam_im * step_size)
    decay_im = magnitude * jnp.sin(lam_im * step_size)
    modulus = lam_re * lam_re + lam_im * lam_im
    hold_re = ((decay_re - 1.0) * lam_re + decay_im * lam_im) / modulus
    hold_im = (decay_im * lam_re - (decay_re - 1.0) * lam_im) / modulus
    drive_re = hold_re[:, None, :] * map_re - hold_im[:, None, :] * map_im
    drive_im = hold_re[:, None, :] * map_im + hold_im[:, None, :] * map_re
    push_re = jnp.einsum('bgc,gcn->bgn', inputs, drive_re, precision=HIGH)
    push_im = jnp.einsum('bgc,gcn->bgn', inputs, drive_im, precision=HIGH)
    fresh_re = decay_re * old_re - decay_im * old_im + push_re
    fresh_im = decay_re * old_im + decay_im * old_re + push_im
    readout = jnp.einsum('bgn,gcn->bgc', fresh_re, read_re, precision=HIGH) - jnp.einsum('bgn,gcn->bgc', fresh_im, read_im, precision=HIGH) + skip_weight * inputs
    return (readout, fresh_re, fresh_im)

def reference(tokens, norm_gain, w_in, w_gate, decay_rate, frequency, log_step, map_re, map_im, read_re, read_im, skip_weight, w_out, state_re, state_im):
    hidden = tokens
    all_re = []
    all_im = []
    for layer in range(LAYERS):
        floats = hidden.astype(jnp.float32)
        inv_scale = lax.rsqrt(lax.optimization_barrier(jnp.mean(floats * floats, axis=-1, keepdims=True)) + EPSILON)
        normed = (floats * inv_scale * norm_gain[layer]).astype(jnp.bfloat16)
        projected = jnp.dot(normed, w_in[layer], preferred_element_type=jnp.float32).astype(jnp.bfloat16)
        gate = jnp.dot(normed, w_gate[layer], preferred_element_type=jnp.float32).astype(jnp.bfloat16)
        rows = projected.shape[0]
        inputs = projected.astype(jnp.float32).reshape(rows, GROUPS, GROUP_CH)
        readout, fresh_re, fresh_im = state_update(inputs, state_re[layer], state_im[layer], decay_rate[layer], frequency[layer], log_step[layer], map_re[layer], map_im[layer], read_re[layer], read_im[layer], skip_weight[layer])
        activated = jax.nn.gelu(readout.reshape(rows, WIDTH))
        mixer = (activated * jax.nn.sigmoid(gate.astype(jnp.float32))).astype(jnp.bfloat16)
        mixed = jnp.dot(mixer, w_out[layer], preferred_element_type=jnp.float32)
        hidden = (floats + mixed).astype(jnp.bfloat16)
        all_re.append(fresh_re)
        all_im.append(fresh_im)
    return (hidden, jnp.stack(all_re), jnp.stack(all_im))
```

```python
import jax
import jax.numpy as jnp
from jax import lax
from jax.experimental import pallas as pl
from jax.experimental.pallas import tpu as pltpu
from jax.sharding import PartitionSpec as P

EPSILON = 1e-06
HIGH = lax.Precision.HIGHEST
F32 = jnp.float32
BF16 = jnp.bfloat16


SAME_CORE = [[2 * y + c for y in range(8)] for c in range(2)]
PARTNER = [(i, i ^ 1) for i in range(16)]


def along_y(shard):
    copies = jnp.broadcast_to(shard, (8, *shard.shape))
    return lax.all_to_all(copies, "dp", split_axis=0, concat_axis=0, tiled=True, axis_index_groups=SAME_CORE)


def to_partner(array):
    return lax.ppermute(array, "dp", PARTNER)


def over_tp(copies):
    return lax.all_to_all(copies, "tp", split_axis=0, concat_axis=0, tiled=True)


def mixer_kernel(core, x, gain, w_own, w_other, drive, read, decay_re, decay_im, skip, old_re, old_im, mixed, new_re, new_im):
    wide = x[...].astype(F32)
    square = jnp.sum(jnp.sum(wide * wide, axis=0), axis=1, keepdims=True)
    inv_scale = lax.rsqrt(square * (1.0 / 4096) + EPSILON)
    c = core[0]
    total = jnp.zeros((16, 128), F32)
    for weights, side in ((w_own, c), (w_other, 1 - c)):
        for y in range(8):
            t = 4 * y + 2 * side
            left = (x[t].astype(F32) * inv_scale * gain[pl.ds(t, 1), :]).astype(BF16)
            right = (x[t + 1].astype(F32) * inv_scale * gain[pl.ds(t + 1, 1), :]).astype(BF16)
            rows = jnp.concatenate([left, right], axis=1)
            total += lax.dot_general(rows, weights[y], (((1,), (1,)), ((), ())), preferred_element_type=F32)
    both = total.astype(BF16).astype(F32)
    push = jnp.dot(both, drive[...], precision=HIGH, preferred_element_type=F32)
    d_re, d_im = decay_re[...], decay_im[...]
    o_re, o_im = old_re[...], old_im[...]
    f_re = d_re * o_re - d_im * o_im + push[:, :256]
    f_im = d_re * o_im + d_im * o_re + push[:, 256:]
    new_re[...] = f_re
    new_im[...] = f_im
    fresh = jnp.concatenate([f_re, f_im], axis=1)
    readout = lax.dot_general(fresh, read[...], (((1,), (1,)), ((), ())), precision=HIGH, preferred_element_type=F32)
    readout = readout + skip[...] * both
    gate = pltpu.roll(both, 64, axis=1)
    mixer = (jax.nn.gelu(readout) * jax.nn.sigmoid(gate)).astype(BF16).astype(F32)
    packed = (mixer[:8] + pltpu.roll(mixer[8:], 64, axis=1)).astype(BF16)
    mixed[...] = jnp.broadcast_to(packed[None], mixed.shape)


def out_kernel(core, mixed, w_own, w_other, before, *outs):
    c = core[0]
    low = lax.broadcasted_iota(jnp.int32, (8, 128), 1) < 64
    total = jnp.zeros((16, 128), F32)
    for weights, side in ((w_own, c), (w_other, 1 - c)):
        for y in range(8):
            t = 4 * y + 2 * side
            a = mixed[t].astype(F32)
            b = mixed[t + 1].astype(F32)
            upper = jnp.where(low, a, pltpu.roll(b, 64, axis=1))
            lower = jnp.where(low, pltpu.roll(a, 64, axis=1), b)
            rows = jnp.concatenate([upper, lower], axis=0).astype(BF16)
            total += jnp.dot(rows, weights[y], preferred_element_type=F32)
    hidden = (before[...].astype(F32) + total).astype(BF16)
    outs[0][...] = hidden
    if len(outs) > 1:
        outs[1][...] = jnp.broadcast_to(hidden[None], outs[1].shape)


def whole(array):
    return pl.BlockSpec(array.shape, lambda *_: (0,) * array.ndim)


def mixer_call(core, x, gain, w_own, w_other, small):
    args = (x, gain, w_own, w_other, *small)
    specs = [pl.BlockSpec(memory_space=pltpu.SMEM)] + [whole(a) for a in args]
    for at in (3, 4):
        specs[at] = pl.BlockSpec((8, 128, 256), lambda *_: (0, 0, 0))
    return pl.pallas_call(
        mixer_kernel,
        grid=(1,),
        in_specs=specs,
        out_specs=[pl.BlockSpec((32, 8, 128), lambda *_: (0, 0, 0)), pl.BlockSpec((16, 256), lambda *_: (0, 0)), pl.BlockSpec((16, 256), lambda *_: (0, 0))],
        out_shape=[jax.ShapeDtypeStruct((32, 8, 128), BF16), jax.ShapeDtypeStruct((16, 256), F32), jax.ShapeDtypeStruct((16, 256), F32)],
        name="mixer_step",
    )(core, *args)


def out_call(core, mixed, w_own, w_other, before, last, at):
    out_shape = [jax.ShapeDtypeStruct((16, 128), BF16)]
    out_specs = [pl.BlockSpec((16, 128), lambda *_: (0, 0))]
    if not last:
        out_shape.append(jax.ShapeDtypeStruct((32, 16, 128), BF16))
        out_specs.append(pl.BlockSpec((32, 16, 128), lambda *_: (0, 0, 0)))
    block = pl.BlockSpec((8, 128, 128), lambda *_: (0, 0, at))
    return pl.pallas_call(
        out_kernel,
        grid=(1,),
        in_specs=[pl.BlockSpec(memory_space=pltpu.SMEM), whole(mixed), block, block, whole(before)],
        out_specs=out_specs,
        out_shape=out_shape,
        name="out_step",
    )(core, mixed, w_own, w_other, before)


def blocks(array):
    layers, groups, channels, n = array.shape
    rows = array.reshape(layers, groups * channels, n)
    tiled = jnp.concatenate([rows] * groups, axis=2)
    row = lax.broadcasted_iota(jnp.int32, tiled.shape, 1) // channels
    col = lax.broadcasted_iota(jnp.int32, tiled.shape, 2) // n
    return jnp.pad(jnp.where(row == col, tiled, 0.0), ((0, 0), (0, 64), (0, 0)))


def local(tokens, norm_gain, w_in, w_gate, decay_rate, frequency, log_step, map_re, map_im, read_re, read_im, skip_weight, w_out, state_re, state_im):
    core = (lax.axis_index("dp") % 2).astype(jnp.int32).reshape(1)
    in_t = jnp.concatenate([w_in.transpose(0, 2, 1), w_gate.transpose(0, 2, 1)], axis=1)

    own_in0 = along_y(in_t[0])
    gathered = over_tp(jnp.broadcast_to(tokens, (32, 16, 128)))
    own_out0 = along_y(w_out[0])
    own_1 = along_y(jnp.concatenate([in_t[1], w_out[1]], axis=1))

    lam_re = -decay_rate
    step_size = jnp.exp(log_step)[:, :, None]
    magnitude = jnp.exp(lam_re * step_size)
    decay_re = magnitude * jnp.cos(frequency * step_size)
    decay_im = magnitude * jnp.sin(frequency * step_size)
    modulus = lam_re * lam_re + frequency * frequency
    hold_re = ((decay_re - 1.0) * lam_re + decay_im * frequency) / modulus
    hold_im = (decay_im * lam_re - (decay_re - 1.0) * frequency) / modulus
    drive_re = hold_re[:, :, None, :] * map_re - hold_im[:, :, None, :] * map_im
    drive_im = hold_re[:, :, None, :] * map_im + hold_im[:, :, None, :] * map_re
    drive = jnp.concatenate([blocks(drive_re), blocks(drive_im)], axis=2)
    read = jnp.concatenate([blocks(read_re), blocks(-read_im)], axis=2)
    skip = jnp.pad(skip_weight.reshape(2, 1, 64), ((0, 0), (0, 0), (0, 64)))
    decay_re, decay_im = decay_re.reshape(2, 1, 256), decay_im.reshape(2, 1, 256)
    old_re, old_im = state_re.reshape(2, 16, 256), state_im.reshape(2, 16, 256)
    gain = norm_gain.reshape(2, 32, 128)
    small = [(drive[l], read[l], decay_re[l], decay_im[l], skip[l], old_re[l], old_im[l]) for l in range(2)]

    mixed, re0, im0 = mixer_call(core, gathered, gain[0], own_in0, to_partner(own_in0), small[0])
    hidden, copies = out_call(core, over_tp(mixed), own_out0, to_partner(own_out0), tokens, False, 0)
    other_1 = to_partner(own_1)
    mixed, re1, im1 = mixer_call(core, over_tp(copies), gain[1], own_1, other_1, small[1])
    hidden = out_call(core, over_tp(mixed), own_1, other_1, hidden, True, 2)[0]
    new_re = jnp.stack([re0, re1]).reshape(state_re.shape)
    new_im = jnp.stack([im0, im1]).reshape(state_im.shape)
    return (hidden, new_re, new_im)


def solution(mesh):
    return jax.shard_map(
        local,
        mesh=mesh,
        in_specs=(
            P("dp", "tp"),
            P(),
            P(None, "dp", "tp"),
            P(None, "dp", "tp"),
            P(None, "tp", None),
            P(None, "tp", None),
            P(None, "tp"),
            P(None, "tp", None, None),
            P(None, "tp", None, None),
            P(None, "tp", None, None),
            P(None, "tp", None, None),
            P(None, "tp", None),
            P(None, "dp", "tp"),
            P(None, "dp", "tp", None),
            P(None, "dp", "tp", None),
        ),
        out_specs=(P("dp", "tp"), P(None, "dp", "tp", None), P(None, "dp", "tp", None)),
        check_vma=False,
    )
```

```python
import functools

import jax
import jax.numpy as jnp
from jax import lax
from jax.experimental import pallas as pl
from jax.experimental.pallas import tpu as pltpu
from jax.sharding import PartitionSpec as P


EPSILON = 1e-06
HIGH = lax.Precision.HIGHEST
F32 = jnp.float32
BF16 = jnp.bfloat16


PARTNER = [(i, i ^ 1) for i in range(16)]
SAME_CORE = [[2 * y + c for y in range(8)] for c in range(2)]
ROUND = [(2 * y, 2 * ((y + 1) % 8)) for y in range(8)] + [(2 * y + 1, 2 * ((y - 1) % 8) + 1) for y in range(8)]


def to_partner(array):
    return lax.ppermute(array, "dp", PARTNER)


def along_y(copies):
    return lax.all_to_all(copies, "dp", split_axis=0, concat_axis=0, tiled=True, axis_index_groups=SAME_CORE)


def behind(array, *others):
    return lax.optimization_barrier((array, *others))[0]


def round_step(piece):
    return lax.ppermute(piece, "dp", ROUND)


def block_of(here, i):
    y, c = here >> 1, here & 1
    k = i // 2
    step = k if k < 5 else 4 - k
    core = c if (i % 2 == 1) == (k >= 5) else 1 - c
    return 2 * ((y + (2 * c - 1) * step) & 7) + core


def shards_of(layer, here, pieces):
    if layer == 0:
        return [(2 * (i % 8) + ((here & 1) ^ (i // 8)), pieces[i // 8], i % 8) for i in range(16)]
    ring = [(block_of(here, i), pieces[i // 2], i % 2) for i in range(10)]
    return ring + [(block_of(here, i), pieces[5], i - 10) for i in range(10, 16)]


def over_tp(copies):
    return lax.all_to_all(copies, "tp", split_axis=0, concat_axis=0, tiled=True)


def loaded(kernel, count):
    def body(*refs):
        sources, sems = refs[:count], refs[-1]
        outs, local = refs[count : -count - 1], refs[-count - 1 : -1]
        copies = [pltpu.make_async_copy(a, b, sems.at[i]) for i, (a, b) in enumerate(zip(sources, local))]
        for copy in copies:
            copy.start()
        for copy in copies:
            copy.wait()
        kernel(*local, *outs)

    return body


def send_kernel(w_in, w_gate, w_out, first, second):
    for y in range(8):
        first[y, 0:64, 0:256] = w_in[0]
        first[y, 64:128, 0:256] = w_gate[0]
        first[y, :, 256:384] = w_out[0]
    second[0:64, 0:256] = w_in[1]
    second[64:128, 0:256] = w_gate[1]
    second[:, 256:384] = w_out[1]


def copy_kernel(tokens, *rest):
    rest[-1][...] = jnp.broadcast_to(tokens[...][None], rest[-1].shape)


def prepare_kernel(gains, decay_rate, frequency, log_step, map_re, map_im, read_re, read_im, skip_weight, state_re, state_im, gain, drive, read, decay, skip, old):
    drive[...] = jnp.zeros(drive.shape, F32)
    read[...] = jnp.zeros(read.shape, F32)
    skip[...] = jnp.zeros(skip.shape, F32)
    for t in range(32):
        gain[:, t, :] = gains[:, 128 * t : 128 * t + 128]
    for l in range(2):
        lam_re = -decay_rate[l]
        lam_im = frequency[l]
        step_size = jnp.exp(log_step[l])
        magnitude = jnp.exp(lam_re * step_size)
        decay_re = magnitude * jnp.cos(lam_im * step_size)
        decay_im = magnitude * jnp.sin(lam_im * step_size)
        modulus = lam_re * lam_re + lam_im * lam_im
        hold_re = ((decay_re - 1.0) * lam_re + decay_im * lam_im) / modulus
        hold_im = (decay_im * lam_re - (decay_re - 1.0) * lam_im) / modulus
        for g in range(4):
            rows, at = slice(16 * g, 16 * g + 16), 64 * g
            h_re, h_im = hold_re[g : g + 1], hold_im[g : g + 1]
            m_re, m_im = map_re[l, g], map_im[l, g]
            drive[l, rows, at : at + 64] = h_re * m_re - h_im * m_im
            drive[l, rows, at + 256 : at + 320] = h_re * m_im + h_im * m_re
            read[l, rows, at : at + 64] = read_re[l, g]
            read[l, rows, at + 256 : at + 320] = -read_im[l, g]
            decay[l, 0:1, at : at + 64] = decay_re[g : g + 1]
            decay[l, 1:2, at : at + 64] = decay_im[g : g + 1]
            skip[l, 0:1, 16 * g : 16 * g + 16] = skip_weight[l, g : g + 1]
            old[l, 0, :, at : at + 64] = state_re[l, :, g, :]
            old[l, 1, :, at : at + 64] = state_im[l, :, g, :]


def mixer_kernel(layer, here, x, gain, drive_far, read_far, decay, skip, old, *rest):
    pieces, (mixed, fresh_out, drive, read, sems) = rest[:-5], rest[-5:]
    get_drive = pltpu.make_async_copy(drive_far.at[layer], drive, sems.at[0])
    get_read = pltpu.make_async_copy(read_far.at[layer], read, sems.at[1])
    get_drive.start()
    get_read.start()
    wide = x[...].astype(F32)
    square = jnp.sum(jnp.sum(wide * wide, axis=0), axis=1, keepdims=True)
    inv_scale = lax.rsqrt(square * (1.0 / 4096) + EPSILON)
    total = jnp.zeros((16, 128), F32)
    for block, array, at in shards_of(layer, here[0], pieces):
        t = 2 * block
        left = (x[t].astype(F32) * inv_scale * gain[layer, pl.ds(t, 1), :]).astype(BF16)
        right = (x[t + 1].astype(F32) * inv_scale * gain[layer, pl.ds(t + 1, 1), :]).astype(BF16)
        rows = jnp.concatenate([left, right], axis=1)
        total += lax.dot_general(rows, array[at, :, 0:256], (((1,), (1,)), ((), ())), preferred_element_type=F32)
    both = total.astype(BF16).astype(F32)
    get_drive.wait()
    push = jnp.dot(both, drive[...], precision=HIGH, preferred_element_type=F32)
    d_re, d_im = decay[layer, 0:1], decay[layer, 1:2]
    o_re, o_im = old[layer, 0], old[layer, 1]
    f_re = d_re * o_re - d_im * o_im + push[:, :256]
    f_im = d_re * o_im + d_im * o_re + push[:, 256:]
    fresh = jnp.concatenate([f_re, f_im], axis=1)
    fresh_out[...] = fresh
    get_read.wait()
    readout = lax.dot_general(fresh, read[...], (((1,), (1,)), ((), ())), precision=HIGH, preferred_element_type=F32)
    readout = readout + skip[layer] * both
    gate = pltpu.roll(both, 64, axis=1)
    mixer = (jax.nn.gelu(readout) * jax.nn.sigmoid(gate)).astype(BF16).astype(F32)
    packed = (mixer[:8] + pltpu.roll(mixer[8:], 64, axis=1)).astype(BF16)
    mixed[...] = jnp.broadcast_to(packed[None], mixed.shape)


def out_kernel(layer, here, mixed, before, *rest):
    count = 2 if layer == 0 else 6
    pieces, outs = rest[:count], rest[count:]
    low = lax.broadcasted_iota(jnp.int32, (8, 128), 1) < 64
    total = jnp.zeros((16, 128), F32)
    for block, array, at in shards_of(layer, here[0], pieces):
        t = 2 * block
        a = mixed[t].astype(F32)
        b = mixed[t + 1].astype(F32)
        upper = jnp.where(low, a, pltpu.roll(b, 64, axis=1))
        lower = jnp.where(low, pltpu.roll(a, 64, axis=1), b)
        rows = jnp.concatenate([upper, lower], axis=0).astype(BF16)
        total += jnp.dot(rows, array[at, :, 256:384], preferred_element_type=F32)
    hidden = (before[...].astype(F32) + total).astype(BF16)
    if layer == 0:
        outs[0][...] = hidden
        outs[1][...] = jnp.broadcast_to(hidden[None], outs[1].shape)
        return
    fresh, (out, new_re, new_im) = outs[:2], outs[2:]
    out[...] = hidden
    for l in range(2):
        for g in range(4):
            new_re[l, :, g, :] = fresh[l][:, 64 * g : 64 * g + 64]
            new_im[l, :, g, :] = fresh[l][:, 64 * g + 256 : 64 * g + 320]


VMEM = pl.BlockSpec(memory_space=pltpu.VMEM)
SMEM = pl.BlockSpec(memory_space=pltpu.SMEM)


def close(*arrays):
    return [pltpu.with_memory_space_constraint(a, pltpu.VMEM) for a in arrays]


def run(kernel, args, shapes, near=(), smem=0):
    return pl.pallas_call(
        kernel,
        in_specs=[SMEM] * smem + [VMEM] * (len(args) - smem),
        out_specs=[VMEM] * len(shapes),
        out_shape=[pltpu.VMEM(*s) if i in near else jax.ShapeDtypeStruct(*s) for i, s in enumerate(shapes)],
        compiler_params=pltpu.CompilerParams(vmem_limit_bytes=16 << 20),
    )(*args)


def run_loaded(kernel, args, shapes, near=()):
    args = [pltpu.with_memory_space_constraint(a, pltpu.HBM) for a in args]
    return pl.pallas_call(
        loaded(kernel, len(args)),
        in_specs=[pl.BlockSpec(memory_space=pltpu.HBM)] * len(args),
        out_specs=[VMEM] * len(shapes),
        out_shape=[pltpu.VMEM(*s) if i in near else jax.ShapeDtypeStruct(*s) for i, s in enumerate(shapes)],
        scratch_shapes=[pltpu.VMEM(a.shape, a.dtype) for a in args] + [pltpu.SemaphoreType.DMA((len(args),))],
        compiler_params=pltpu.CompilerParams(vmem_limit_bytes=16 << 20),
    )(*args)


def mixer_call(layer, here, x, small, pieces):
    gain, drive, read, decay, skip, old = small
    args = [here, *close(x, gain), drive, read, *close(decay, skip, old, *pieces)]
    specs = [SMEM] + [VMEM] * (len(args) - 1)
    for at in (3, 4):
        args[at] = pltpu.with_memory_space_constraint(args[at], pltpu.HBM)
        specs[at] = pl.BlockSpec(memory_space=pltpu.HBM)
    return pl.pallas_call(
        functools.partial(mixer_kernel, layer),
        in_specs=specs,
        out_specs=[VMEM] * 2,
        out_shape=[jax.ShapeDtypeStruct((32, 8, 128), BF16), pltpu.VMEM((16, 512), F32)],
        scratch_shapes=[pltpu.VMEM((128, 512), F32)] * 2 + [pltpu.SemaphoreType.DMA((2,))],
        compiler_params=pltpu.CompilerParams(vmem_limit_bytes=16 << 20),
        name="mixer_step",
    )(*args)


def copy_call(tokens, *after):
    return pl.pallas_call(
        copy_kernel,
        in_specs=[VMEM] + [pl.BlockSpec(memory_space=pl.ANY)] * len(after),
        out_specs=VMEM,
        out_shape=jax.ShapeDtypeStruct((32, 16, 128), BF16),
        compiler_params=pltpu.CompilerParams(vmem_limit_bytes=16 << 20),
        name="copy_step",
    )(tokens, *after)


def local(tokens, norm_gain, w_in, w_gate, decay_rate, frequency, log_step, map_re, map_im, read_re, read_im, skip_weight, w_out, state_re, state_im):
    here = lax.axis_index("dp").astype(jnp.int32).reshape(1)
    first, second = run_loaded(
        send_kernel,
        (w_in.transpose(0, 2, 1), w_gate.transpose(0, 2, 1), w_out),
        [((8, 128, 384), BF16), ((128, 384), BF16)],
        (1,),
    )
    small = run_loaded(
        prepare_kernel,
        (norm_gain, decay_rate, frequency, log_step[:, :, None], map_re, map_im, read_re, read_im, skip_weight, state_re, state_im),
        [((2, 32, 128), F32), ((2, 128, 512), F32), ((2, 128, 512), F32), ((2, 2, 256), F32), ((2, 1, 128), F32), ((2, 2, 16, 256), F32)],
        (0, 3, 4, 5),
    )
    w_own = along_y(first)
    pieces = [jnp.stack([second, to_partner(second)])]
    pieces.append(round_step(pieces[0]))
    w_other = to_partner(w_own)
    copies = copy_call(tokens, small[3])
    gathered = over_tp(copies)
    pieces.append(round_step(behind(pieces[1], w_own)))
    mixed, fresh0 = mixer_call(0, here, gathered, small, (w_own, w_other))
    pieces.append(round_step(behind(pieces[2], fresh0)))
    mixed = over_tp(mixed)
    shapes = [((16, 128), BF16), ((32, 16, 128), BF16)]
    hidden, copies = run(functools.partial(out_kernel, 0), (here, *close(mixed), tokens, *close(w_own, w_other)), shapes, (0,), 1)
    pieces.append(round_step(behind(pieces[3], hidden)))
    pieces.append(to_partner(behind(jnp.concatenate(pieces[1:4]), hidden)))
    mixed, fresh1 = mixer_call(1, here, over_tp(copies), small, pieces)
    shapes = [((16, 128), BF16), (state_re.shape, F32), (state_im.shape, F32)]
    args = (here, *close(over_tp(mixed), hidden, *pieces, fresh0, fresh1))
    return tuple(run(functools.partial(out_kernel, 1), args, shapes, (), 1))


def solution(mesh):
    return jax.shard_map(
        local,
        mesh=mesh,
        in_specs=(
            P("dp", "tp"),
            P(),
            P(None, "dp", "tp"),
            P(None, "dp", "tp"),
            P(None, "tp", None),
            P(None, "tp", None),
            P(None, "tp"),
            P(None, "tp", None, None),
            P(None, "tp", None, None),
            P(None, "tp", None, None),
            P(None, "tp", None, None),
            P(None, "tp", None),
            P(None, "dp", "tp"),
            P(None, "dp", "tp", None),
            P(None, "dp", "tp", None),
        ),
        out_specs=(P("dp", "tp"), P(None, "dp", "tp", None), P(None, "dp", "tp", None)),
        check_vma=False,
    )
```

```python
import functools

import jax
import jax.numpy as jnp
from jax import lax
from jax.experimental import pallas as pl
from jax.experimental.pallas import tpu as pltpu
from jax.sharding import PartitionSpec as P


EPSILON = 1e-06
HIGH = lax.Precision.HIGHEST
F32 = jnp.float32
BF16 = jnp.bfloat16


PARTNER = [(i, i ^ 1) for i in range(16)]


def to_partner(array):
    return lax.ppermute(array, "dp", PARTNER)


def from_y(array, k):
    pairs = [(2 * ((y + k) % 8), 2 * y) for y in range(8)] + [(2 * ((y - k) % 8) + 1, 2 * y + 1) for y in range(8)]
    return lax.ppermute(array, "dp", pairs)


def behind(array, *others):
    return lax.optimization_barrier((array, *others))[0]


def shards_of(here, pieces):
    y, c = here >> 1, here & 1
    way = 1 - 2 * c
    order = [(0, 0, 0), (0, 2, 1), (1, 0, 2), (1, 2, 3), (2, 0, 4), (3, 0, -1), (3, 2, -2), (3, 4, -3)]
    found = []
    for array, at, k in order:
        first = c if array < 3 else 1 - c
        base = 2 * ((y + way * k) & 7)
        found += [(base + first, pieces[array], at), (base + 1 - first, pieces[array], at + 1)]
    return found


def over_tp(copies):
    return lax.all_to_all(copies, "tp", split_axis=0, concat_axis=0, tiled=True)


def loaded(kernel, count):
    def body(*refs):
        sources, sems = refs[:count], refs[-1]
        outs, local = refs[count : -count - 1], refs[-count - 1 : -1]
        copies = [pltpu.make_async_copy(a, b, sems.at[i]) for i, (a, b) in enumerate(zip(sources, local))]
        for copy in copies:
            copy.start()
        for copy in copies:
            copy.wait()
        kernel(*local, *outs)

    return body


def send_kernel(w_in, w_gate, w_out, shard):
    for l in range(2):
        at = 384 * l
        shard[0, 0:64, at : at + 256] = w_in[l]
        shard[0, 64:128, at : at + 256] = w_gate[l]
        shard[0, :, at + 256 : at + 384] = w_out[l]


def stack_kernel(pair, near, tokens, both0, both1, copies):
    for l, both in ((0, both0), (1, both1)):
        lanes = slice(384 * l, 384 * l + 384)
        both[0:2] = pair[:, :, lanes]
        both[2:4] = near[:, :, lanes]
    copies[...] = jnp.broadcast_to(tokens[...][None], copies.shape)


def join_kernel(both, far, joined, last):
    joined[0:2] = both[2:4]
    joined[2:6] = far[...]
    last[...] = far[2:4]


def prepare_kernel(gains, decay_rate, frequency, log_step, map_re, map_im, read_re, read_im, skip_weight, state_re, state_im, gain, drive, read, decay, skip, old):
    drive[...] = jnp.zeros(drive.shape, F32)
    read[...] = jnp.zeros(read.shape, F32)
    skip[...] = jnp.zeros(skip.shape, F32)
    for t in range(32):
        gain[:, t, :] = gains[:, 128 * t : 128 * t + 128]
    for l in range(2):
        lam_re = -decay_rate[l]
        lam_im = frequency[l]
        step_size = jnp.exp(log_step[l])
        magnitude = jnp.exp(lam_re * step_size)
        decay_re = magnitude * jnp.cos(lam_im * step_size)
        decay_im = magnitude * jnp.sin(lam_im * step_size)
        modulus = lam_re * lam_re + lam_im * lam_im
        hold_re = ((decay_re - 1.0) * lam_re + decay_im * lam_im) / modulus
        hold_im = (decay_im * lam_re - (decay_re - 1.0) * lam_im) / modulus
        for g in range(4):
            rows, at = slice(16 * g, 16 * g + 16), 64 * g
            h_re, h_im = hold_re[g : g + 1], hold_im[g : g + 1]
            m_re, m_im = map_re[l, g], map_im[l, g]
            drive[l, rows, at : at + 64] = h_re * m_re - h_im * m_im
            drive[l, rows, at + 256 : at + 320] = h_re * m_im + h_im * m_re
            read[l, rows, at : at + 64] = read_re[l, g]
            read[l, rows, at + 256 : at + 320] = -read_im[l, g]
            decay[l, 0:1, at : at + 64] = decay_re[g : g + 1]
            decay[l, 1:2, at : at + 64] = decay_im[g : g + 1]
            skip[l, 0:1, 16 * g : 16 * g + 16] = skip_weight[l, g : g + 1]
            old[l, 0, :, at : at + 64] = state_re[l, :, g, :]
            old[l, 1, :, at : at + 64] = state_im[l, :, g, :]


def mixer_kernel(layer, here, x, gain, drive_far, read_far, decay, skip, old, *rest):
    pieces, (mixed, fresh_out, drive, read, sems) = rest[:-5], rest[-5:]
    get_drive = pltpu.make_async_copy(drive_far.at[layer], drive, sems.at[0])
    get_read = pltpu.make_async_copy(read_far.at[layer], read, sems.at[1])
    get_drive.start()
    get_read.start()
    wide = x[...].astype(F32)
    square = jnp.sum(jnp.sum(wide * wide, axis=0), axis=1, keepdims=True)
    inv_scale = lax.rsqrt(square * (1.0 / 4096) + EPSILON)
    total = jnp.zeros((16, 128), F32)
    for block, array, at in shards_of(here[0], pieces):
        t = 2 * block
        left = (x[t].astype(F32) * inv_scale * gain[layer, pl.ds(t, 1), :]).astype(BF16)
        right = (x[t + 1].astype(F32) * inv_scale * gain[layer, pl.ds(t + 1, 1), :]).astype(BF16)
        rows = jnp.concatenate([left, right], axis=1)
        total += lax.dot_general(rows, array[at, :, 0:256], (((1,), (1,)), ((), ())), preferred_element_type=F32)
    both = total.astype(BF16).astype(F32)
    get_drive.wait()
    push = jnp.dot(both, drive[...], precision=HIGH, preferred_element_type=F32)
    d_re, d_im = decay[layer, 0:1], decay[layer, 1:2]
    o_re, o_im = old[layer, 0], old[layer, 1]
    f_re = d_re * o_re - d_im * o_im + push[:, :256]
    f_im = d_re * o_im + d_im * o_re + push[:, 256:]
    fresh = jnp.concatenate([f_re, f_im], axis=1)
    fresh_out[...] = fresh
    get_read.wait()
    readout = lax.dot_general(fresh, read[...], (((1,), (1,)), ((), ())), precision=HIGH, preferred_element_type=F32)
    readout = readout + skip[layer] * both
    gate = pltpu.roll(both, 64, axis=1)
    mixer = (jax.nn.gelu(readout) * jax.nn.sigmoid(gate)).astype(BF16).astype(F32)
    packed = (mixer[:8] + pltpu.roll(mixer[8:], 64, axis=1)).astype(BF16)
    mixed[...] = jnp.broadcast_to(packed[None], mixed.shape)


def out_kernel(layer, here, mixed, before, *rest):
    pieces, outs = rest[:4], rest[4:]
    low = lax.broadcasted_iota(jnp.int32, (8, 128), 1) < 64
    total = jnp.zeros((16, 128), F32)
    for block, array, at in shards_of(here[0], pieces):
        t = 2 * block
        a = mixed[t].astype(F32)
        b = mixed[t + 1].astype(F32)
        upper = jnp.where(low, a, pltpu.roll(b, 64, axis=1))
        lower = jnp.where(low, pltpu.roll(a, 64, axis=1), b)
        rows = jnp.concatenate([upper, lower], axis=0).astype(BF16)
        total += jnp.dot(rows, array[at, :, 256:384], preferred_element_type=F32)
    hidden = (before[...].astype(F32) + total).astype(BF16)
    if layer == 0:
        outs[0][...] = hidden
        outs[1][...] = jnp.broadcast_to(hidden[None], outs[1].shape)
        return
    fresh, (out, new_re, new_im) = outs[:2], outs[2:]
    out[...] = hidden
    for l in range(2):
        for g in range(4):
            new_re[l, :, g, :] = fresh[l][:, 64 * g : 64 * g + 64]
            new_im[l, :, g, :] = fresh[l][:, 64 * g + 256 : 64 * g + 320]


VMEM = pl.BlockSpec(memory_space=pltpu.VMEM)
SMEM = pl.BlockSpec(memory_space=pltpu.SMEM)


def close(*arrays):
    return [pltpu.with_memory_space_constraint(a, pltpu.VMEM) for a in arrays]


def run(kernel, args, shapes, near=(), smem=0):
    return pl.pallas_call(
        kernel,
        in_specs=[SMEM] * smem + [VMEM] * (len(args) - smem),
        out_specs=[VMEM] * len(shapes),
        out_shape=[pltpu.VMEM(*s) if i in near else jax.ShapeDtypeStruct(*s) for i, s in enumerate(shapes)],
        compiler_params=pltpu.CompilerParams(vmem_limit_bytes=16 << 20),
    )(*args)


def run_loaded(kernel, args, shapes, near=()):
    args = [pltpu.with_memory_space_constraint(a, pltpu.HBM) for a in args]
    return pl.pallas_call(
        loaded(kernel, len(args)),
        in_specs=[pl.BlockSpec(memory_space=pltpu.HBM)] * len(args),
        out_specs=[VMEM] * len(shapes),
        out_shape=[pltpu.VMEM(*s) if i in near else jax.ShapeDtypeStruct(*s) for i, s in enumerate(shapes)],
        scratch_shapes=[pltpu.VMEM(a.shape, a.dtype) for a in args] + [pltpu.SemaphoreType.DMA((len(args),))],
        compiler_params=pltpu.CompilerParams(vmem_limit_bytes=16 << 20),
    )(*args)


def mixer_call(layer, here, x, small, pieces):
    gain, drive, read, decay, skip, old = small
    args = [here, *close(x, gain), drive, read, *close(decay, skip, old, *pieces)]
    specs = [SMEM] + [VMEM] * (len(args) - 1)
    for at in (3, 4):
        args[at] = pltpu.with_memory_space_constraint(args[at], pltpu.HBM)
        specs[at] = pl.BlockSpec(memory_space=pltpu.HBM)
    return pl.pallas_call(
        functools.partial(mixer_kernel, layer),
        in_specs=specs,
        out_specs=[VMEM] * 2,
        out_shape=[jax.ShapeDtypeStruct((32, 8, 128), BF16), pltpu.VMEM((16, 512), F32)],
        scratch_shapes=[pltpu.VMEM((128, 512), F32)] * 2 + [pltpu.SemaphoreType.DMA((2,))],
        compiler_params=pltpu.CompilerParams(vmem_limit_bytes=16 << 20),
        name="mixer_step",
    )(*args)


def local(tokens, norm_gain, w_in, w_gate, decay_rate, frequency, log_step, map_re, map_im, read_re, read_im, skip_weight, w_out, state_re, state_im):
    here = lax.axis_index("dp").astype(jnp.int32).reshape(1)
    shard = run_loaded(
        send_kernel, (w_in.transpose(0, 2, 1), w_gate.transpose(0, 2, 1), w_out), [((1, 128, 768), BF16)], (0,)
    )[0]
    small = run_loaded(
        prepare_kernel,
        (norm_gain, decay_rate, frequency, log_step[:, :, None], map_re, map_im, read_re, read_im, skip_weight, state_re, state_im),
        [((2, 32, 128), F32), ((2, 128, 512), F32), ((2, 128, 512), F32), ((2, 2, 256), F32), ((2, 1, 128), F32), ((2, 2, 16, 256), F32)],
        (0, 3, 4, 5),
    )
    pair = jnp.concatenate([shard, to_partner(shard)])
    near = from_y(pair, 1)
    shapes = [((4, 128, 384), BF16)] * 2 + [((32, 16, 128), BF16)]
    both0, both1, copies = run(stack_kernel, close(pair, near) + [tokens], shapes, range(2))

    def pieces_of(both):
        far = from_y(both, 2)
        shapes = [((6, 128, 384), BF16), ((2, 128, 384), BF16)]
        joined, last = run(join_kernel, close(both, far), shapes, (0, 1))
        last = from_y(last, 1)
        across = to_partner(joined)
        return [both, far, last, across]

    gathered = over_tp(copies)
    first = pieces_of(both0)
    mixed, fresh0 = mixer_call(0, here, gathered, small, first)
    second = pieces_of(behind(both1, fresh0))
    mixed = over_tp(mixed)
    shapes = [((16, 128), BF16), ((32, 16, 128), BF16)]
    hidden, copies = run(functools.partial(out_kernel, 0), (here, *close(mixed), tokens, *close(*first)), shapes, (0,), 1)
    gathered = over_tp(copies)
    mixed, fresh1 = mixer_call(1, here, gathered, small, second)
    shapes = [((16, 128), BF16), (state_re.shape, F32), (state_im.shape, F32)]
    args = (here, *close(over_tp(mixed), hidden, *second, fresh0, fresh1))
    return tuple(run(functools.partial(out_kernel, 1), args, shapes, (), 1))


def solution(mesh):
    return jax.shard_map(
        local,
        mesh=mesh,
        in_specs=(
            P("dp", "tp"),
            P(),
            P(None, "dp", "tp"),
            P(None, "dp", "tp"),
            P(None, "tp", None),
            P(None, "tp", None),
            P(None, "tp"),
            P(None, "tp", None, None),
            P(None, "tp", None, None),
            P(None, "tp", None, None),
            P(None, "tp", None, None),
            P(None, "tp", None),
            P(None, "dp", "tp"),
            P(None, "dp", "tp", None),
            P(None, "dp", "tp", None),
        ),
        out_specs=(P("dp", "tp"), P(None, "dp", "tp", None), P(None, "dp", "tp", None)),
        check_vma=False,
    )
```

```python
import functools

import jax
import jax.numpy as jnp
from jax import lax
from jax.experimental import pallas as pl
from jax.experimental.pallas import tpu as pltpu
from jax.sharding import PartitionSpec as P


EPSILON = 1e-06
F32 = jnp.float32
BF16 = jnp.bfloat16


PARTNER = [(i, i ^ 1) for i in range(16)]


def to_partner(array):
    return lax.ppermute(array, "dp", PARTNER)


def from_y(array, k):
    pairs = [(2 * ((y + k) % 8), 2 * y) for y in range(8)] + [(2 * ((y - k) % 8) + 1, 2 * y + 1) for y in range(8)]
    return lax.ppermute(array, "dp", pairs)


def shards_of(here, pieces):
    y, c = here >> 1, here & 1
    way = 1 - 2 * c
    order = [(0, 0, 0), (0, 2, 1), (1, 0, 2), (1, 2, 3), (2, 0, 4), (3, 0, -1), (3, 2, -2), (3, 4, -3)]
    found = []
    for array, at, k in order:
        first = c if array < 3 else 1 - c
        base = 2 * ((y + way * k) & 7)
        found += [(base + first, pieces[array], at), (base + 1 - first, pieces[array], at + 1)]
    return found


def over_tp(copies):
    return lax.all_to_all(copies, "tp", split_axis=0, concat_axis=0, tiled=True)


def loaded(kernel, count, outs_count):
    def body(*refs):
        sources, outs = refs[:count], refs[count : count + outs_count]
        local, sems, own = refs[count + outs_count : 2 * count + outs_count], refs[2 * count + outs_count], refs[2 * count + outs_count + 1 :]
        copies = [pltpu.make_async_copy(a, b, sems.at[i]) for i, (a, b) in enumerate(zip(sources, local))]
        for copy in copies:
            copy.start()
        for copy in copies:
            copy.wait()
        kernel(*local, *outs, *own)

    return body


def send_kernel(w_in, w_gate, w_out, shard):
    for l in range(2):
        at = 384 * l
        shard[0, 0:64, at : at + 256] = w_in[l]
        shard[0, 64:128, at : at + 256] = w_gate[l]
        shard[0, :, at + 256 : at + 384] = w_out[l]


def stack_kernel(pair, near, both0, both1):
    for l, both in ((0, both0), (1, both1)):
        lanes = slice(384 * l, 384 * l + 384)
        both[0:2] = pair[:, :, lanes]
        both[2:4] = near[:, :, lanes]


def halves(array):
    upper = array.astype(BF16)
    return upper, (array - upper.astype(F32)).astype(BF16)


def join_kernel(both, far, joined, last):
    joined[0:2] = both[2:4]
    joined[2:6] = far[...]
    last[...] = far[2:4]


def prepare_kernel(gains, decay_rate, frequency, log_step, map_re, map_im, read_re, read_im, skip_weight, state_re, state_im, tokens, gain, drive_far, read_far, decay, skip, old, copies, drive, read, drive_parts, read_parts, sems):
    copies[...] = jnp.broadcast_to(tokens[...][None], copies.shape)
    drive[...] = jnp.zeros(drive.shape, F32)
    read[...] = jnp.zeros(read.shape, F32)
    skip[...] = jnp.zeros(skip.shape, F32)
    for t in range(32):
        gain[:, t, :] = gains[:, 128 * t : 128 * t + 128]
    for l in range(2):
        lam_re = -decay_rate[l]
        lam_im = frequency[l]
        group = lax.broadcasted_iota(jnp.int32, (4, 64), 0)
        step_size = jnp.zeros((4, 64), F32)
        for g in range(4):
            step_size = jnp.where(group == g, log_step[l : l + 1, g : g + 1], step_size)
        step_size = jnp.exp(step_size)
        magnitude = jnp.exp(lam_re * step_size)
        decay_re = magnitude * jnp.cos(lam_im * step_size)
        decay_im = magnitude * jnp.sin(lam_im * step_size)
        modulus = lam_re * lam_re + lam_im * lam_im
        hold_re = ((decay_re - 1.0) * lam_re + decay_im * lam_im) / modulus
        hold_im = (decay_im * lam_re - (decay_re - 1.0) * lam_im) / modulus
        for g in range(4):
            rows, at = slice(16 * g, 16 * g + 16), 64 * g
            h_re, h_im = hold_re[g : g + 1], hold_im[g : g + 1]
            m_re, m_im = map_re[l, g], map_im[l, g]
            drive[l, rows, at : at + 64] = h_re * m_re - h_im * m_im
            drive[l, rows, at + 256 : at + 320] = h_re * m_im + h_im * m_re
            read[l, rows, at : at + 64] = read_re[l, g]
            read[l, rows, at + 256 : at + 320] = -read_im[l, g]
            decay[l, 0:1, at : at + 64] = decay_re[g : g + 1]
            decay[l, 1:2, at : at + 64] = decay_im[g : g + 1]
            skip[l, 0:1, 16 * g : 16 * g + 16] = skip_weight[l, g : g + 1]
            old[l, 0, :, at : at + 64] = state_re[l, :, g, :]
            old[l, 1, :, at : at + 64] = state_im[l, :, g, :]
    moves = []
    for i, (full, parts, far) in enumerate(((drive, drive_parts, drive_far), (read, read_parts, read_far))):
        parts[:, :, 0:512], parts[:, :, 512:1024] = halves(full[...])
        moves.append(pltpu.make_async_copy(parts, far, sems.at[i]))
        moves[i].start()
    for move in moves:
        move.wait()


def mixer_kernel(layer, here, x, gain, drive_far, read_far, decay, skip, old, *rest):
    pieces, (mixed, fresh_out, drive, read, sems) = rest[:-5], rest[-5:]
    get_drive = pltpu.make_async_copy(drive_far.at[layer], drive, sems.at[0])
    get_read = pltpu.make_async_copy(read_far.at[layer], read, sems.at[1])
    get_drive.start()
    get_read.start()
    wide = x[...].astype(F32)
    square = jnp.sum(jnp.sum(wide * wide, axis=0), axis=1, keepdims=True)
    inv_scale = lax.rsqrt(square * (1.0 / 4096) + EPSILON)
    turned = jnp.zeros((128, 16), F32)
    for block, array, at in shards_of(here[0], pieces):
        t = 2 * block
        left = (x[t].astype(F32) * inv_scale * gain[layer, pl.ds(t, 1), :]).astype(BF16)
        right = (x[t + 1].astype(F32) * inv_scale * gain[layer, pl.ds(t + 1, 1), :]).astype(BF16)
        rows = jnp.concatenate([left, right], axis=1)
        turned += lax.dot_general(array[at, :, 0:256], rows, (((1,), (1,)), ((), ())), preferred_element_type=F32)
    both = turned.T.astype(BF16).astype(F32)
    get_drive.wait()
    parts = jnp.dot(both.astype(BF16), drive[...], preferred_element_type=F32)
    push = parts[:, :512] + parts[:, 512:]
    d_re, d_im = decay[layer, 0:1], decay[layer, 1:2]
    o_re, o_im = old[layer, 0], old[layer, 1]
    f_re = d_re * o_re - d_im * o_im + push[:, :256]
    f_im = d_re * o_im + d_im * o_re + push[:, 256:]
    fresh = jnp.concatenate([f_re, f_im], axis=1)
    fresh_out[...] = fresh
    get_read.wait()
    upper, lower = halves(fresh)
    contract = (((1,), (1,)), ((), ()))
    parts = lax.dot_general(jnp.concatenate([upper, lower]), read[:, :512], contract, preferred_element_type=F32)
    readout = parts[:16] + parts[16:] + lax.dot_general(upper, read[:, 512:], contract, preferred_element_type=F32)
    readout = readout + skip[layer] * both
    gate = pltpu.roll(both, 64, axis=1)
    mixer = (jax.nn.gelu(readout) * jax.nn.sigmoid(gate)).astype(BF16).astype(F32)
    packed = (mixer[:8] + pltpu.roll(mixer[8:], 64, axis=1)).astype(BF16)
    mixed[...] = jnp.broadcast_to(packed[None], mixed.shape)


def out_kernel(layer, here, mixed, before, *rest):
    pieces, outs = rest[:4], rest[4:]
    low = lax.broadcasted_iota(jnp.int32, (8, 128), 1) < 64
    total = jnp.zeros((16, 128), F32)
    for block, array, at in shards_of(here[0], pieces):
        t = 2 * block
        a = mixed[t].astype(F32)
        b = mixed[t + 1].astype(F32)
        upper = jnp.where(low, a, pltpu.roll(b, 64, axis=1))
        lower = jnp.where(low, pltpu.roll(a, 64, axis=1), b)
        rows = jnp.concatenate([upper, lower], axis=0).astype(BF16)
        total += jnp.dot(rows, array[at, :, 256:384], preferred_element_type=F32)
    hidden = (before[...].astype(F32) + total).astype(BF16)
    if layer == 0:
        outs[0][...] = hidden
        outs[1][...] = jnp.broadcast_to(hidden[None], outs[1].shape)
        return
    fresh, (out, new_re, new_im) = outs[:2], outs[2:]
    out[...] = hidden
    for l in range(2):
        for g in range(4):
            new_re[l, :, g, :] = fresh[l][:, 64 * g : 64 * g + 64]
            new_im[l, :, g, :] = fresh[l][:, 64 * g + 256 : 64 * g + 320]


VMEM = pl.BlockSpec(memory_space=pltpu.VMEM)
SMEM = pl.BlockSpec(memory_space=pltpu.SMEM)


def close(*arrays):
    return [pltpu.with_memory_space_constraint(a, pltpu.VMEM) for a in arrays]


def run(kernel, args, shapes, near=(), smem=0):
    return pl.pallas_call(
        kernel,
        in_specs=[SMEM] * smem + [VMEM] * (len(args) - smem),
        out_specs=[VMEM] * len(shapes),
        out_shape=[pltpu.VMEM(*s) if i in near else jax.ShapeDtypeStruct(*s) for i, s in enumerate(shapes)],
        compiler_params=pltpu.CompilerParams(vmem_limit_bytes=16 << 20),
    )(*args)


def run_loaded(kernel, args, shapes, near=(), far=(), scratch=()):
    args = [pltpu.with_memory_space_constraint(a, pltpu.HBM) for a in args]
    return pl.pallas_call(
        loaded(kernel, len(args), len(shapes)),
        in_specs=[pl.BlockSpec(memory_space=pltpu.HBM)] * len(args),
        out_specs=[pl.BlockSpec(memory_space=pltpu.HBM) if i in far else VMEM for i in range(len(shapes))],
        out_shape=[pltpu.VMEM(*s) if i in near else pltpu.HBM(*s) if i in far else jax.ShapeDtypeStruct(*s) for i, s in enumerate(shapes)],
        scratch_shapes=[pltpu.VMEM(a.shape, a.dtype) for a in args] + [pltpu.SemaphoreType.DMA((len(args),)), *scratch],
        compiler_params=pltpu.CompilerParams(vmem_limit_bytes=16 << 20),
    )(*args)


def mixer_call(layer, here, x, small, pieces):
    gain, drive, read, decay, skip, old = small
    args = [here, *close(x, gain), drive, read, *close(decay, skip, old, *pieces)]
    specs = [SMEM] + [VMEM] * (len(args) - 1)
    for at in (3, 4):
        args[at] = pltpu.with_memory_space_constraint(args[at], pltpu.HBM)
        specs[at] = pl.BlockSpec(memory_space=pltpu.HBM)
    return pl.pallas_call(
        functools.partial(mixer_kernel, layer),
        in_specs=specs,
        out_specs=[VMEM] * 2,
        out_shape=[jax.ShapeDtypeStruct((32, 8, 128), BF16), pltpu.VMEM((16, 512), F32)],
        scratch_shapes=[pltpu.VMEM((128, 1024), BF16)] * 2 + [pltpu.SemaphoreType.DMA((2,))],
        compiler_params=pltpu.CompilerParams(vmem_limit_bytes=16 << 20),
        name="mixer_step",
    )(*args)


def local(tokens, norm_gain, w_in, w_gate, decay_rate, frequency, log_step, map_re, map_im, read_re, read_im, skip_weight, w_out, state_re, state_im):
    here = lax.axis_index("dp").astype(jnp.int32).reshape(1)
    shard = run_loaded(
        send_kernel, (w_in.transpose(0, 2, 1), w_gate.transpose(0, 2, 1), w_out), [((1, 128, 768), BF16)], (0,)
    )[0]
    *small, copies = run_loaded(
        prepare_kernel,
        (norm_gain, decay_rate, frequency, log_step, map_re, map_im, read_re, read_im, skip_weight, state_re, state_im, tokens),
        [((2, 32, 128), F32), ((2, 128, 1024), BF16), ((2, 128, 1024), BF16), ((2, 2, 256), F32), ((2, 1, 128), F32), ((2, 2, 16, 256), F32), ((32, 16, 128), BF16)],
        (0, 3, 4, 5),
        (1, 2),
        [pltpu.VMEM((2, 128, 512), F32)] * 2 + [pltpu.VMEM((2, 128, 1024), BF16)] * 2 + [pltpu.SemaphoreType.DMA((2,))],
    )
    pair = jnp.concatenate([shard, to_partner(shard)])
    near = from_y(pair, 1)
    both0, both1 = run(stack_kernel, close(pair, near), [((4, 128, 384), BF16)] * 2, range(2))

    def pieces_of(both):
        far = from_y(both, 2)
        shapes = [((6, 128, 384), BF16), ((2, 128, 384), BF16)]
        joined, last = run(join_kernel, close(both, far), shapes, (0, 1))
        last = from_y(last, 1)
        across = to_partner(joined)
        return [both, far, last, across]

    gathered = over_tp(copies)
    first = pieces_of(both0)
    mixed, fresh0 = mixer_call(0, here, gathered, small, first)
    second = pieces_of(both1)
    mixed = over_tp(mixed)
    shapes = [((16, 128), BF16), ((32, 16, 128), BF16)]
    hidden, copies = run(functools.partial(out_kernel, 0), (here, *close(mixed), tokens, *close(*first)), shapes, (0,), 1)
    gathered = over_tp(copies)
    mixed, fresh1 = mixer_call(1, here, gathered, small, second)
    shapes = [((16, 128), BF16), (state_re.shape, F32), (state_im.shape, F32)]
    args = (here, *close(over_tp(mixed), hidden, *second, fresh0, fresh1))
    return tuple(run(functools.partial(out_kernel, 1), args, shapes, (), 1))


def solution(mesh):
    return jax.shard_map(
        local,
        mesh=mesh,
        in_specs=(
            P("dp", "tp"),
            P(),
            P(None, "dp", "tp"),
            P(None, "dp", "tp"),
            P(None, "tp", None),
            P(None, "tp", None),
            P(None, "tp"),
            P(None, "tp", None, None),
            P(None, "tp", None, None),
            P(None, "tp", None, None),
            P(None, "tp", None, None),
            P(None, "tp", None),
            P(None, "dp", "tp"),
            P(None, "dp", "tp", None),
            P(None, "dp", "tp", None),
        ),
        out_specs=(P("dp", "tp"), P(None, "dp", "tp", None), P(None, "dp", "tp", None)),
        check_vma=False,
    )
```

```python
import functools

import jax
import jax.numpy as jnp
from jax import lax
from jax.experimental import pallas as pl
from jax.experimental.pallas import tpu as pltpu
from jax.sharding import PartitionSpec as P


EPSILON = 1e-06
F32 = jnp.float32
BF16 = jnp.bfloat16


PARTNER = [(i, i ^ 1) for i in range(16)]
DIAGONAL = [(2 * ((y + 1) % 8) + 1, 2 * y) for y in range(8)] + [(2 * ((y - 1) % 8), 2 * y + 1) for y in range(8)]


def to_partner(array):
    return lax.ppermute(array, "dp", PARTNER)


def from_y(array, k):
    pairs = [(2 * ((y + k) % 8), 2 * y) for y in range(8)] + [(2 * ((y - k) % 8) + 1, 2 * y + 1) for y in range(8)]
    return lax.ppermute(array, "dp", pairs)


def shards_of(here, pieces):
    y, c = here >> 1, here & 1
    found = []
    for array, core in ((pieces[0], c), (pieces[1], 1 - c)):
        for i in range(8):
            side = core if i % 2 == 0 else 1 - core
            found.append((2 * ((y + (1 - 2 * core) * ((i + 1) // 2)) & 7) + side, array, i))
    return found


def over_tp(copies):
    return lax.all_to_all(copies, "tp", split_axis=0, concat_axis=0, tiled=True)


def loaded(kernel, count, outs_count):
    def body(*refs):
        sources, outs = refs[:count], refs[count : count + outs_count]
        local, sems, own = refs[count + outs_count : 2 * count + outs_count], refs[2 * count + outs_count], refs[2 * count + outs_count + 1 :]
        copies = [pltpu.make_async_copy(a, b, sems.at[i]) for i, (a, b) in enumerate(zip(sources, local))]
        for copy in copies:
            copy.start()
        for copy in copies:
            copy.wait()
        kernel(*local, *outs, *own)

    return body


def copy_kernel(tokens, copies):
    copies[...] = jnp.broadcast_to(tokens[...][None], copies.shape)


def send_kernel(w_in, w_gate, w_out, shard):
    for l in range(2):
        at = 384 * l
        shard[0, 0:64, at : at + 256] = w_in[l]
        shard[0, 64:128, at : at + 256] = w_gate[l]
        shard[0, :, at + 256 : at + 384] = w_out[l]


def stack_kernel(pair, near, both0, both1):
    for both, lanes in ((both0, slice(0, 256)), (both1, slice(256, 768))):
        both[0:2] = pair[:, :, lanes]
        both[2:4] = near[:, :, lanes]


def halves(array):
    upper = array.astype(BF16)
    return upper, (array - upper.astype(F32)).astype(BF16)


def join_kernel(both, far, joined):
    joined[0:4] = both[...]
    joined[4:8] = far[...]


def prepare_kernel(gains, decay_rate, frequency, log_step, map_re, map_im, read_re, read_im, skip_weight, state_re, state_im, gain, drive_far, read_far, decay, skip, old, drive, read, drive_parts, read_parts, sems):
    drive[...] = jnp.zeros(drive.shape, F32)
    read[...] = jnp.zeros(read.shape, F32)
    skip[...] = jnp.zeros(skip.shape, F32)
    for t in range(32):
        gain[:, t, :] = gains[:, 128 * t : 128 * t + 128]
    for l in range(2):
        lam_re = -decay_rate[l]
        lam_im = frequency[l]
        group = lax.broadcasted_iota(jnp.int32, (4, 64), 0)
        step_size = jnp.zeros((4, 64), F32)
        for g in range(4):
            step_size = jnp.where(group == g, log_step[l : l + 1, g : g + 1], step_size)
        step_size = jnp.exp(step_size)
        magnitude = jnp.exp(lam_re * step_size)
        decay_re = magnitude * jnp.cos(lam_im * step_size)
        decay_im = magnitude * jnp.sin(lam_im * step_size)
        modulus = lam_re * lam_re + lam_im * lam_im
        hold_re = ((decay_re - 1.0) * lam_re + decay_im * lam_im) / modulus
        hold_im = (decay_im * lam_re - (decay_re - 1.0) * lam_im) / modulus
        for g in range(4):
            rows, at = slice(16 * g, 16 * g + 16), 64 * g
            h_re, h_im = hold_re[g : g + 1], hold_im[g : g + 1]
            m_re, m_im = map_re[l, g], map_im[l, g]
            drive[l, rows, at : at + 64] = h_re * m_re - h_im * m_im
            drive[l, rows, at + 256 : at + 320] = h_re * m_im + h_im * m_re
            read[l, rows, at : at + 64] = read_re[l, g]
            read[l, rows, at + 256 : at + 320] = -read_im[l, g]
            decay[l, 0:1, at : at + 64] = decay_re[g : g + 1]
            decay[l, 1:2, at : at + 64] = decay_im[g : g + 1]
            skip[l, 0:1, 16 * g : 16 * g + 16] = skip_weight[l, g : g + 1]
            old[l, 0, :, at : at + 64] = state_re[l, :, g, :]
            old[l, 1, :, at : at + 64] = state_im[l, :, g, :]
    moves = []
    for i, (full, parts, far) in enumerate(((drive, drive_parts, drive_far), (read, read_parts, read_far))):
        parts[:, :, 0:512], parts[:, :, 512:1024] = halves(full[...])
        moves.append(pltpu.make_async_copy(parts, far, sems.at[i]))
        moves[i].start()
    for move in moves:
        move.wait()


def mixer_kernel(layer, here, x, gain, drive_far, read_far, decay, skip, old, *rest):
    pieces, (mixed, fresh_out, drive, read, sems) = rest[:-5], rest[-5:]
    get_drive = pltpu.make_async_copy(drive_far.at[layer], drive, sems.at[0])
    get_read = pltpu.make_async_copy(read_far.at[layer], read, sems.at[1])
    get_drive.start()
    get_read.start()
    wide = x[...].astype(F32)
    square = jnp.sum(jnp.sum(wide * wide, axis=0), axis=1, keepdims=True)
    inv_scale = lax.rsqrt(square * (1.0 / 4096) + EPSILON)
    turned = jnp.zeros((128, 16), F32)
    for block, array, at in shards_of(here[0], pieces):
        t = 2 * block
        left = (x[t].astype(F32) * inv_scale * gain[layer, pl.ds(t, 1), :]).astype(BF16)
        right = (x[t + 1].astype(F32) * inv_scale * gain[layer, pl.ds(t + 1, 1), :]).astype(BF16)
        rows = jnp.concatenate([left, right], axis=1)
        turned += lax.dot_general(array[at, :, 128 * layer : 128 * layer + 256], rows, (((1,), (1,)), ((), ())), preferred_element_type=F32)
    both = turned.T.astype(BF16).astype(F32)
    get_drive.wait()
    parts = jnp.dot(both.astype(BF16), drive[...], preferred_element_type=F32)
    push = parts[:, :512] + parts[:, 512:]
    d_re, d_im = decay[layer, 0:1], decay[layer, 1:2]
    o_re, o_im = old[layer, 0], old[layer, 1]
    f_re = d_re * o_re - d_im * o_im + push[:, :256]
    f_im = d_re * o_im + d_im * o_re + push[:, 256:]
    fresh = jnp.concatenate([f_re, f_im], axis=1)
    fresh_out[...] = fresh
    get_read.wait()
    upper, lower = halves(fresh)
    contract = (((1,), (1,)), ((), ()))
    parts = lax.dot_general(jnp.concatenate([upper, lower]), read[:, :512], contract, preferred_element_type=F32)
    readout = parts[:16] + parts[16:] + lax.dot_general(upper, read[:, 512:], contract, preferred_element_type=F32)
    readout = readout + skip[layer] * both
    gate = pltpu.roll(both, 64, axis=1)
    mixer = (jax.nn.gelu(readout) * jax.nn.sigmoid(gate)).astype(BF16).astype(F32)
    packed = (mixer[:8] + pltpu.roll(mixer[8:], 64, axis=1)).astype(BF16)
    mixed[...] = jnp.broadcast_to(packed[None], mixed.shape)


def out_kernel(layer, here, mixed, before, *rest):
    pieces, outs = rest[:2], rest[2:]
    low = lax.broadcasted_iota(jnp.int32, (8, 128), 1) < 64
    total = jnp.zeros((16, 128), F32)
    for block, array, at in shards_of(here[0], pieces):
        t = 2 * block
        a = mixed[t].astype(F32)
        b = mixed[t + 1].astype(F32)
        upper = jnp.where(low, a, pltpu.roll(b, 64, axis=1))
        lower = jnp.where(low, pltpu.roll(a, 64, axis=1), b)
        rows = jnp.concatenate([upper, lower], axis=0).astype(BF16)
        total += jnp.dot(rows, array[at, :, 384 * layer : 384 * layer + 128], preferred_element_type=F32)
    hidden = (before[...].astype(F32) + total).astype(BF16)
    if layer == 0:
        outs[0][...] = hidden
        outs[1][...] = jnp.broadcast_to(hidden[None], outs[1].shape)
        return
    fresh, (out, new_re, new_im) = outs[:2], outs[2:]
    out[...] = hidden
    for l in range(2):
        for g in range(4):
            new_re[l, :, g, :] = fresh[l][:, 64 * g : 64 * g + 64]
            new_im[l, :, g, :] = fresh[l][:, 64 * g + 256 : 64 * g + 320]


VMEM = pl.BlockSpec(memory_space=pltpu.VMEM)
SMEM = pl.BlockSpec(memory_space=pltpu.SMEM)


def close(*arrays):
    return [pltpu.with_memory_space_constraint(a, pltpu.VMEM) for a in arrays]


def run(kernel, args, shapes, near=(), smem=0):
    return pl.pallas_call(
        kernel,
        in_specs=[SMEM] * smem + [VMEM] * (len(args) - smem),
        out_specs=[VMEM] * len(shapes),
        out_shape=[pltpu.VMEM(*s) if i in near else jax.ShapeDtypeStruct(*s) for i, s in enumerate(shapes)],
        compiler_params=pltpu.CompilerParams(vmem_limit_bytes=16 << 20),
    )(*args)


def run_loaded(kernel, args, shapes, near=(), far=(), scratch=()):
    args = [pltpu.with_memory_space_constraint(a, pltpu.HBM) for a in args]
    return pl.pallas_call(
        loaded(kernel, len(args), len(shapes)),
        in_specs=[pl.BlockSpec(memory_space=pltpu.HBM)] * len(args),
        out_specs=[pl.BlockSpec(memory_space=pltpu.HBM) if i in far else VMEM for i in range(len(shapes))],
        out_shape=[pltpu.VMEM(*s) if i in near else pltpu.HBM(*s) if i in far else jax.ShapeDtypeStruct(*s) for i, s in enumerate(shapes)],
        scratch_shapes=[pltpu.VMEM(a.shape, a.dtype) for a in args] + [pltpu.SemaphoreType.DMA((len(args),)), *scratch],
        compiler_params=pltpu.CompilerParams(vmem_limit_bytes=16 << 20),
    )(*args)


def mixer_call(layer, here, x, small, pieces):
    gain, drive, read, decay, skip, old = small
    args = [here, *close(x, gain), drive, read, *close(decay, skip, old, *pieces)]
    specs = [SMEM] + [VMEM] * (len(args) - 1)
    for at in (3, 4):
        args[at] = pltpu.with_memory_space_constraint(args[at], pltpu.HBM)
        specs[at] = pl.BlockSpec(memory_space=pltpu.HBM)
    return pl.pallas_call(
        functools.partial(mixer_kernel, layer),
        in_specs=specs,
        out_specs=[VMEM] * 2,
        out_shape=[jax.ShapeDtypeStruct((32, 8, 128), BF16), pltpu.VMEM((16, 512), F32)],
        scratch_shapes=[pltpu.VMEM((128, 1024), BF16)] * 2 + [pltpu.SemaphoreType.DMA((2,))],
        compiler_params=pltpu.CompilerParams(vmem_limit_bytes=16 << 20),
        name="mixer_step",
    )(*args)


def local(tokens, norm_gain, w_in, w_gate, decay_rate, frequency, log_step, map_re, map_im, read_re, read_im, skip_weight, w_out, state_re, state_im):
    here = lax.axis_index("dp").astype(jnp.int32).reshape(1)
    shard = run_loaded(
        send_kernel, (w_in.transpose(0, 2, 1), w_gate.transpose(0, 2, 1), w_out), [((1, 128, 768), BF16)], (0,)
    )[0]
    small = run_loaded(
        prepare_kernel,
        (norm_gain, decay_rate, frequency, log_step, map_re, map_im, read_re, read_im, skip_weight, state_re, state_im),
        [((2, 32, 128), F32), ((2, 128, 1024), BF16), ((2, 128, 1024), BF16), ((2, 2, 256), F32), ((2, 1, 128), F32), ((2, 2, 16, 256), F32)],
        (0, 3, 4, 5),
        (1, 2),
        [pltpu.VMEM((2, 128, 512), F32)] * 2 + [pltpu.VMEM((2, 128, 1024), BF16)] * 2 + [pltpu.SemaphoreType.DMA((2,))],
    )
    copies = run_loaded(copy_kernel, (tokens,), [((32, 16, 128), BF16)])[0]
    pair = jnp.concatenate([shard, lax.ppermute(shard, "dp", DIAGONAL)])
    near = from_y(pair, 1)
    both0, both1 = run(stack_kernel, close(pair, near), [((4, 128, 256), BF16), ((4, 128, 512), BF16)], range(2))

    def pieces_of(both):
        far = from_y(both, 2)
        joined = run(join_kernel, close(both, far), [((8, 128, both.shape[2]), BF16)], (0,))[0]
        across = to_partner(joined)
        return [joined, across]

    gathered = over_tp(copies)
    first = pieces_of(both0)
    mixed, fresh0 = mixer_call(0, here, gathered, small, first)
    second = pieces_of(both1)
    mixed = over_tp(mixed)
    shapes = [((16, 128), BF16), ((32, 16, 128), BF16)]
    hidden, copies = run(functools.partial(out_kernel, 0), (here, *close(mixed), tokens, *close(*second)), shapes, (0,), 1)
    gathered = over_tp(copies)
    mixed, fresh1 = mixer_call(1, here, gathered, small, second)
    shapes = [((16, 128), BF16), (state_re.shape, F32), (state_im.shape, F32)]
    args = (here, *close(over_tp(mixed), hidden, *second, fresh0, fresh1))
    return tuple(run(functools.partial(out_kernel, 1), args, shapes, (), 1))


def solution(mesh):
    return jax.shard_map(
        local,
        mesh=mesh,
        in_specs=(
            P("dp", "tp"),
            P(),
            P(None, "dp", "tp"),
            P(None, "dp", "tp"),
            P(None, "tp", None),
            P(None, "tp", None),
            P(None, "tp"),
            P(None, "tp", None, None),
            P(None, "tp", None, None),
            P(None, "tp", None, None),
            P(None, "tp", None, None),
            P(None, "tp", None),
            P(None, "dp", "tp"),
            P(None, "dp", "tp", None),
            P(None, "dp", "tp", None),
        ),
        out_specs=(P("dp", "tp"), P(None, "dp", "tp", None), P(None, "dp", "tp", None)),
        check_vma=False,
    )
```

```python
import functools

import jax
import jax.numpy as jnp
from jax import lax
from jax.experimental import pallas as pl
from jax.experimental.pallas import tpu as pltpu
from jax.sharding import PartitionSpec as P


EPSILON = 1e-06
F32 = jnp.float32
BF16 = jnp.bfloat16


PARTNER = [(i, i ^ 1) for i in range(16)]
DIAGONAL = [(2 * ((y + 1) % 8) + 1, 2 * y) for y in range(8)] + [(2 * ((y - 1) % 8), 2 * y + 1) for y in range(8)]


def to_partner(array):
    return lax.ppermute(array, "dp", PARTNER)


def from_y(array, k):
    pairs = [(2 * ((y + k) % 8), 2 * y) for y in range(8)] + [(2 * ((y - k) % 8) + 1, 2 * y + 1) for y in range(8)]
    return lax.ppermute(array, "dp", pairs)


def shards_of(here, pieces):
    y, c = here >> 1, here & 1
    found = []
    for array, core in ((pieces[0], c), (pieces[1], 1 - c)):
        for i in range(8):
            side = core if i % 2 == 0 else 1 - core
            found.append((2 * ((y + (1 - 2 * core) * ((i + 1) // 2)) & 7) + side, array, i))
    return found


def over_tp(copies):
    return lax.all_to_all(copies, "tp", split_axis=0, concat_axis=0, tiled=True)


def loaded(kernel, count, outs_count):
    def body(*refs):
        sources, outs = refs[:count], refs[count : count + outs_count]
        local, sems, own = refs[count + outs_count : 2 * count + outs_count], refs[2 * count + outs_count], refs[2 * count + outs_count + 1 :]
        copies = [pltpu.make_async_copy(a, b, sems.at[i]) for i, (a, b) in enumerate(zip(sources, local))]
        for copy in copies:
            copy.start()
        for copy in copies:
            copy.wait()
        kernel(*local, *outs, *own)

    return body


def copy_kernel(tokens, copies):
    copies[...] = jnp.broadcast_to(tokens[...][None], copies.shape)


def send_kernel(w_in, w_gate, w_out, shard):
    for l in range(2):
        at = 384 * l
        shard[0, 0:64, at : at + 256] = w_in[l]
        shard[0, 64:128, at : at + 256] = w_gate[l]
        shard[0, :, at + 256 : at + 384] = w_out[l]


def stack_kernel(pair, near, both0, both1):
    for both, lanes in ((both0, slice(0, 256)), (both1, slice(256, 768))):
        both[0:2] = pair[:, :, lanes]
        both[2:4] = near[:, :, lanes]


def halves(array):
    upper = array.astype(BF16)
    return upper, (array - upper.astype(F32)).astype(BF16)


def join_kernel(both, far, joined):
    joined[0:4] = both[...]
    joined[4:8] = far[...]


def prepare_kernel(gains, decay_rate, frequency, log_step, map_re, map_im, read_re, read_im, skip_weight, state_re, state_im, gain, drive_far, read_far, decay, skip, old, drive, read, drive_parts, read_parts, sems):
    drive[...] = jnp.zeros(drive.shape, F32)
    read[...] = jnp.zeros(read.shape, F32)
    skip[...] = jnp.zeros(skip.shape, F32)
    for t in range(32):
        gain[:, t, :] = gains[:, 128 * t : 128 * t + 128]
    for l in range(2):
        lam_re = -decay_rate[l]
        lam_im = frequency[l]
        group = lax.broadcasted_iota(jnp.int32, (4, 64), 0)
        step_size = jnp.zeros((4, 64), F32)
        for g in range(4):
            step_size = jnp.where(group == g, log_step[l : l + 1, g : g + 1], step_size)
        step_size = jnp.exp(step_size)
        magnitude = jnp.exp(lam_re * step_size)
        decay_re = magnitude * jnp.cos(lam_im * step_size)
        decay_im = magnitude * jnp.sin(lam_im * step_size)
        modulus = lam_re * lam_re + lam_im * lam_im
        hold_re = ((decay_re - 1.0) * lam_re + decay_im * lam_im) / modulus
        hold_im = (decay_im * lam_re - (decay_re - 1.0) * lam_im) / modulus
        for g in range(4):
            rows, at = slice(16 * g, 16 * g + 16), 64 * g
            h_re, h_im = hold_re[g : g + 1], hold_im[g : g + 1]
            m_re, m_im = map_re[l, g], map_im[l, g]
            drive[l, rows, at : at + 64] = h_re * m_re - h_im * m_im
            drive[l, rows, at + 256 : at + 320] = h_re * m_im + h_im * m_re
            read[l, rows, at : at + 64] = read_re[l, g]
            read[l, rows, at + 256 : at + 320] = -read_im[l, g]
            decay[l, 0:1, at : at + 64] = decay_re[g : g + 1]
            decay[l, 1:2, at : at + 64] = decay_im[g : g + 1]
            skip[l, 0:1, 16 * g : 16 * g + 16] = skip_weight[l, g : g + 1]
            old[l, 0, :, at : at + 64] = state_re[l, :, g, :]
            old[l, 1, :, at : at + 64] = state_im[l, :, g, :]
    moves = []
    for i, (full, parts, far) in enumerate(((drive, drive_parts, drive_far), (read, read_parts, read_far))):
        parts[:, :, 0:512], parts[:, :, 512:1024] = halves(full[...])
        moves.append(pltpu.make_async_copy(parts, far, sems.at[i]))
        moves[i].start()
    for move in moves:
        move.wait()


def scale_of(x):
    wide = x[...].astype(F32)
    square = jnp.sum(jnp.sum(wide * wide, axis=0), axis=1, keepdims=True)
    return lax.rsqrt(square * (1.0 / 4096) + EPSILON)


def project(layer, x, gain, inv_scale, found, turned):
    for block, array, at in found:
        t = 2 * block
        left = (x[t].astype(F32) * inv_scale * gain[layer, pl.ds(t, 1), :]).astype(BF16)
        right = (x[t + 1].astype(F32) * inv_scale * gain[layer, pl.ds(t + 1, 1), :]).astype(BF16)
        rows = jnp.concatenate([left, right], axis=1)
        turned += lax.dot_general(array[at, :, 128 * layer : 128 * layer + 256], rows, (((1,), (1,)), ((), ())), preferred_element_type=F32)
    return turned


def half_kernel(here, x, gain, drive_far, read_far, joined, scale, partial, drive, read, sems):
    copies = [pltpu.make_async_copy(a.at[0], b, sems.at[i]) for i, (a, b) in enumerate(((drive_far, drive), (read_far, read)))]
    for copy in copies:
        copy.start()
    inv_scale = scale_of(x)
    scale[...] = jnp.broadcast_to(inv_scale, scale.shape)
    partial[...] = project(0, x, gain, inv_scale, shards_of(here[0], [joined, joined])[:8], jnp.zeros((128, 16), F32))
    for copy in copies:
        copy.wait()


def rest_kernel(here, x, gain, decay, skip, old, across, scale, partial, drive, read, mixed, fresh_out):
    turned = project(0, x, gain, scale[...], shards_of(here[0], [across, across])[8:], partial[...])
    finish(0, turned, drive, read, decay, skip, old, mixed, fresh_out)


def mixer_kernel(here, x, gain, drive_far, read_far, decay, skip, old, joined, across, mixed, fresh_out, drive, read, sems):
    copies = [pltpu.make_async_copy(a.at[1], b, sems.at[i]) for i, (a, b) in enumerate(((drive_far, drive), (read_far, read)))]
    for copy in copies:
        copy.start()
    turned = project(1, x, gain, scale_of(x), shards_of(here[0], [joined, across]), jnp.zeros((128, 16), F32))
    for copy in copies:
        copy.wait()
    finish(1, turned, drive, read, decay, skip, old, mixed, fresh_out)


def finish(layer, turned, drive, read, decay, skip, old, mixed, fresh_out):
    both = turned.T.astype(BF16).astype(F32)
    parts = jnp.dot(both.astype(BF16), drive[...], preferred_element_type=F32)
    push = parts[:, :512] + parts[:, 512:]
    d_re, d_im = decay[layer, 0:1], decay[layer, 1:2]
    o_re, o_im = old[layer, 0], old[layer, 1]
    f_re = d_re * o_re - d_im * o_im + push[:, :256]
    f_im = d_re * o_im + d_im * o_re + push[:, 256:]
    fresh = jnp.concatenate([f_re, f_im], axis=1)
    fresh_out[...] = fresh
    upper, lower = halves(fresh)
    contract = (((1,), (1,)), ((), ()))
    parts = lax.dot_general(jnp.concatenate([upper, lower]), read[:, :512], contract, preferred_element_type=F32)
    readout = parts[:16] + parts[16:] + lax.dot_general(upper, read[:, 512:], contract, preferred_element_type=F32)
    readout = readout + skip[layer] * both
    gate = pltpu.roll(both, 64, axis=1)
    mixer = (jax.nn.gelu(readout) * jax.nn.sigmoid(gate)).astype(BF16).astype(F32)
    packed = (mixer[:8] + pltpu.roll(mixer[8:], 64, axis=1)).astype(BF16)
    mixed[...] = jnp.broadcast_to(packed[None], mixed.shape)


def out_kernel(layer, here, mixed, before, *rest):
    pieces, outs = rest[:2], rest[2:]
    low = lax.broadcasted_iota(jnp.int32, (8, 128), 1) < 64
    total = jnp.zeros((16, 128), F32)
    for block, array, at in shards_of(here[0], pieces):
        t = 2 * block
        a = mixed[t].astype(F32)
        b = mixed[t + 1].astype(F32)
        upper = jnp.where(low, a, pltpu.roll(b, 64, axis=1))
        lower = jnp.where(low, pltpu.roll(a, 64, axis=1), b)
        rows = jnp.concatenate([upper, lower], axis=0).astype(BF16)
        total += jnp.dot(rows, array[at, :, 384 * layer : 384 * layer + 128], preferred_element_type=F32)
    hidden = (before[...].astype(F32) + total).astype(BF16)
    if layer == 0:
        outs[0][...] = hidden
        outs[1][...] = jnp.broadcast_to(hidden[None], outs[1].shape)
        return
    fresh, (out, new_re, new_im) = outs[:2], outs[2:]
    out[...] = hidden
    for l in range(2):
        for g in range(4):
            new_re[l, :, g, :] = fresh[l][:, 64 * g : 64 * g + 64]
            new_im[l, :, g, :] = fresh[l][:, 64 * g + 256 : 64 * g + 320]


VMEM = pl.BlockSpec(memory_space=pltpu.VMEM)
SMEM = pl.BlockSpec(memory_space=pltpu.SMEM)


def close(*arrays):
    return [pltpu.with_memory_space_constraint(a, pltpu.VMEM) for a in arrays]


def run(kernel, args, shapes, near=(), smem=0):
    return pl.pallas_call(
        kernel,
        in_specs=[SMEM] * smem + [VMEM] * (len(args) - smem),
        out_specs=[VMEM] * len(shapes),
        out_shape=[pltpu.VMEM(*s) if i in near else jax.ShapeDtypeStruct(*s) for i, s in enumerate(shapes)],
        compiler_params=pltpu.CompilerParams(vmem_limit_bytes=16 << 20),
    )(*args)


def run_loaded(kernel, args, shapes, near=(), far=(), scratch=()):
    args = [pltpu.with_memory_space_constraint(a, pltpu.HBM) for a in args]
    return pl.pallas_call(
        loaded(kernel, len(args), len(shapes)),
        in_specs=[pl.BlockSpec(memory_space=pltpu.HBM)] * len(args),
        out_specs=[pl.BlockSpec(memory_space=pltpu.HBM) if i in far else VMEM for i in range(len(shapes))],
        out_shape=[pltpu.VMEM(*s) if i in near else pltpu.HBM(*s) if i in far else jax.ShapeDtypeStruct(*s) for i, s in enumerate(shapes)],
        scratch_shapes=[pltpu.VMEM(a.shape, a.dtype) for a in args] + [pltpu.SemaphoreType.DMA((len(args),)), *scratch],
        compiler_params=pltpu.CompilerParams(vmem_limit_bytes=16 << 20),
    )(*args)


def far_call(kernel, args, far, shapes, near, scratch=()):
    specs = [SMEM] + [VMEM] * (len(args) - 1)
    for at in far:
        args[at] = pltpu.with_memory_space_constraint(args[at], pltpu.HBM)
        specs[at] = pl.BlockSpec(memory_space=pltpu.HBM)
    return pl.pallas_call(
        kernel,
        in_specs=specs,
        out_specs=[VMEM] * len(shapes),
        out_shape=[pltpu.VMEM(*s) if i in near else jax.ShapeDtypeStruct(*s) for i, s in enumerate(shapes)],
        scratch_shapes=[*scratch, pltpu.SemaphoreType.DMA((2,))],
        compiler_params=pltpu.CompilerParams(vmem_limit_bytes=16 << 20),
    )(*args)


MIXED = [((32, 8, 128), BF16), ((16, 512), F32)]


def local(tokens, norm_gain, w_in, w_gate, decay_rate, frequency, log_step, map_re, map_im, read_re, read_im, skip_weight, w_out, state_re, state_im):
    here = lax.axis_index("dp").astype(jnp.int32).reshape(1)
    shard = run_loaded(
        send_kernel, (w_in.transpose(0, 2, 1), w_gate.transpose(0, 2, 1), w_out), [((1, 128, 768), BF16)], (0,)
    )[0]
    small = run_loaded(
        prepare_kernel,
        (norm_gain, decay_rate, frequency, log_step, map_re, map_im, read_re, read_im, skip_weight, state_re, state_im),
        [((2, 32, 128), F32), ((2, 128, 1024), BF16), ((2, 128, 1024), BF16), ((2, 2, 256), F32), ((2, 1, 128), F32), ((2, 2, 16, 256), F32)],
        (0, 3, 4, 5),
        (1, 2),
        [pltpu.VMEM((2, 128, 512), F32)] * 2 + [pltpu.VMEM((2, 128, 1024), BF16)] * 2 + [pltpu.SemaphoreType.DMA((2,))],
    )
    copies = run_loaded(copy_kernel, (tokens,), [((32, 16, 128), BF16)])[0]
    pair = jnp.concatenate([shard, lax.ppermute(shard, "dp", DIAGONAL)])
    near = from_y(pair, 1)
    both0, both1 = run(stack_kernel, close(pair, near), [((4, 128, 256), BF16), ((4, 128, 512), BF16)], range(2))

    def pieces_of(both):
        far = from_y(both, 2)
        joined = run(join_kernel, close(both, far), [((8, 128, both.shape[2]), BF16)], (0,))[0]
        across = to_partner(joined)
        return [joined, across]

    gathered = over_tp(copies)
    first = pieces_of(both0)
    gain, drive, read, decay, skip, old = small
    shapes = [((16, 128), F32), ((128, 16), F32), ((128, 1024), BF16), ((128, 1024), BF16)]
    args = [here, *close(gathered, gain), drive, read, *close(first[0])]
    halfway = far_call(half_kernel, args, (3, 4), shapes, range(4))
    args = (here, *close(gathered, gain, decay, skip, old, first[1], *halfway))
    mixed, fresh0 = run(rest_kernel, args, MIXED, (1,), 1)
    second = pieces_of(both1)
    mixed = over_tp(mixed)
    shapes = [((16, 128), BF16), ((32, 16, 128), BF16)]
    hidden, copies = run(functools.partial(out_kernel, 0), (here, *close(mixed), tokens, *close(*second)), shapes, (0,), 1)
    gathered = over_tp(copies)
    args = [here, *close(gathered, gain), drive, read, *close(decay, skip, old, *second)]
    mixed, fresh1 = far_call(mixer_kernel, args, (3, 4), MIXED, (1,), [pltpu.VMEM((128, 1024), BF16)] * 2)
    shapes = [((16, 128), BF16), (state_re.shape, F32), (state_im.shape, F32)]
    args = (here, *close(over_tp(mixed), hidden, *second, fresh0, fresh1))
    return tuple(run(functools.partial(out_kernel, 1), args, shapes, (), 1))


def solution(mesh):
    return jax.shard_map(
        local,
        mesh=mesh,
        in_specs=(
            P("dp", "tp"),
            P(),
            P(None, "dp", "tp"),
            P(None, "dp", "tp"),
            P(None, "tp", None),
            P(None, "tp", None),
            P(None, "tp"),
            P(None, "tp", None, None),
            P(None, "tp", None, None),
            P(None, "tp", None, None),
            P(None, "tp", None, None),
            P(None, "tp", None),
            P(None, "dp", "tp"),
            P(None, "dp", "tp", None),
            P(None, "dp", "tp", None),
        ),
        out_specs=(P("dp", "tp"), P(None, "dp", "tp", None), P(None, "dp", "tp", None)),
        check_vma=False,
    )
```
